256 devices in a mesh: ep: 32 (over z, x), tp: 8 (over y, core).
Axes of the slice: x: 4, y: 4, z: 8, core: 2. Of those that a mesh axis runs over, the one named last changes fastest.
Arguments:
- tokens: bfloat16 [1024, 2048], P('ep'), may hold values from -24 to 24
- norm_gain: float32 [2048], replicated, may hold values from 0.1 to 1.9
- post_gain: float32 [2048], replicated, may hold values from 0.1 to 1.9
- w_query: bfloat16 [2048, 2048], P(None, 'tp'), may hold values from -0.125 to 0.125
- w_key: bfloat16 [2048, 512], P(None, 'tp'), may hold values from -0.125 to 0.125
- w_value: bfloat16 [2048, 512], P(None, 'tp'), may hold values from -0.125 to 0.125
- w_forget: bfloat16 [2048, 32], replicated, may hold values from -0.25 to 0.25
- w_output: bfloat16 [2048, 2048], P('tp'), may hold values from -0.125 to 0.125
- key_cache: bfloat16 [1024, 8, 64, 1024], P('ep', 'tp'), may hold values from -660 to 660
- value_cache: bfloat16 [1024, 8, 64, 1024], P('ep', 'tp'), may hold values from -6 to 6
- gate_cache: float32 [1024, 32, 1024], P('ep', 'tp'), may hold values from -176.08 to 0, as said below
- lengths: int32 [1024], P('ep'), may hold values from 256 to 1024
- routes: int32 [1024, 2], P('ep'), may hold values from 0 to 31, all different within a row; in each aligned block of 32 rows (0 to 31, 32 to 63, ...) at most 4 rows name the same one
- route_logits: float32 [1024, 2], P('ep'), may hold values from -6 to 6
- w_gate: bfloat16 [32, 2048, 3584], P('ep', None, 'tp'), may hold values from -0.125 to 0.125
- w_up: bfloat16 [32, 2048, 3584], P('ep', None, 'tp'), may hold values from -0.125 to 0.125
- w_down: bfloat16 [32, 3584, 2048], P('ep', 'tp'), may hold values from -0.09375 to 0.09375
Outputs:
- layer_out: bfloat16 [1024, 2048], P('ep', 'tp')
The draws below stay inside these ranges and needn't reach their ends.
Inputs may be any that keep to these rules, and one draw needn't show every extreme that they name: `routes`: each row names 2 different experts. The rows of one index of ep name any one expert at most 4 times, and in every draw some index of ep names some expert exactly 4 times. `gate_cache`: cumulative sums of negative log forget gates along positions: nonincreasing along the last dimension. `lengths`: the new token follows the valid positions of its sequence.
All inputs are finite; a program needn't handle non-finite values.
Results may differ from the reference program's by a relative error of at most 0.011.
Values may be sent and summed in bfloat16 or wider, within the bound.
A program may use at most 64 MiB of HBM per device.

```python
import math
import jax
import jax.numpy as jnp
import numpy as np
from jax import lax

WIDTH = 2048
QUERY_HEADS = 32
HEAD_DIM = 64
KV_HEADS = 8
FFN = 3584
TOPK = 2
TOK_GRP = 32
CACHE_POSITIONS = 1024
SEQUENCE_TOTAL = 1024
EXPERTS = 32
CAP = 4
N_EP = 32
N_TP = 8


def draw_tokens(key, part):
    first, second = jax.random.split(jax.random.fold_in(key, 3))
    row_scale = jnp.exp(jax.random.uniform(first, (SEQUENCE_TOTAL, 1), jnp.float32, jnp.log(0.3), jnp.log(3.0)))
    column_scale = 0.4 * jnp.exp(jnp.log(4.0) * jnp.arange(WIDTH, dtype=jnp.float32) / WIDTH)
    base = jnp.clip(jax.random.normal(second, (SEQUENCE_TOTAL, WIDTH), jnp.float32), -5.0, 5.0)
    return (row_scale * column_scale[None, :] * base).astype(jnp.bfloat16)


def draw_key_cache(key, part):
    first = jax.random.fold_in(jax.random.fold_in(key, 5), 0)
    base = jnp.clip(jax.random.normal(first, (SEQUENCE_TOTAL, KV_HEADS, HEAD_DIM, CACHE_POSITIONS), jnp.float32), -6.0, 6.0)
    return base.astype(jnp.bfloat16)


def draw_gate_cache(key, part):
    key_entries = jax.random.split(jax.random.fold_in(key, 7), 7)
    slow_share = 0.5
    keeps = jax.random.uniform(key_entries[0], (SEQUENCE_TOTAL, QUERY_HEADS, 1), jnp.float32) < slow_share
    slow_total = jax.random.uniform(key_entries[1], (SEQUENCE_TOTAL, QUERY_HEADS, 1), jnp.float32, 0.2, 0.9)
    fast_rate = jnp.exp(jax.random.uniform(key_entries[2], (SEQUENCE_TOTAL, QUERY_HEADS, 1), jnp.float32, jnp.log(0.03), jnp.log(0.1)))
    decay_rate = jnp.where(keeps, slow_total / CACHE_POSITIONS, fast_rate)
    coarse_estimate = jax.random.uniform(key_entries[3], (SEQUENCE_TOTAL, QUERY_HEADS, CACHE_POSITIONS), jnp.float32, 0.3, 1.7)
    cache_position = jnp.arange(CACHE_POSITIONS, dtype=jnp.int32)[None, None, :]
    leading_group = jax.random.randint(key_entries[4], (SEQUENCE_TOTAL, QUERY_HEADS, 1), 0, CACHE_POSITIONS)
    trailing_group = jax.random.randint(key_entries[5], (SEQUENCE_TOTAL, QUERY_HEADS, 1), 0, CACHE_POSITIONS)
    group_length = jax.random.uniform(key_entries[6], (SEQUENCE_TOTAL, QUERY_HEADS, 2), jnp.float32, 0.22, 0.69)
    position_groups = (cache_position == leading_group).astype(jnp.float32) * group_length[:, :, 0:1] + (cache_position == trailing_group).astype(jnp.float32) * group_length[:, :, 1:2]
    decode_steps = -decay_rate * coarse_estimate - position_groups
    return jnp.cumsum(decode_steps, axis=-1).astype(jnp.float32)


def with_ends(entries, rng, least, high):
    index_at = [jax.random.randint(jax.random.fold_in(rng, axis), (), 0, length) for axis, length in enumerate(entries.shape)]
    widest = entries.shape.index(max(entries.shape))
    beside = index_at[:widest] + [(index_at[widest] + 1) % entries.shape[widest]] + index_at[widest + 1:]
    return entries.at[tuple(index_at)].set(least).at[tuple(beside)].set(high)


def block_levels(stream_key, extent, cuts, low, largest):
    loudness, own = 1.0, jax.random.fold_in(stream_key, 6)
    for position, blocks in cuts:
        draws = jnp.exp(jax.random.uniform(jax.random.fold_in(own, position), (blocks,), jnp.float32, low / len(cuts), largest / len(cuts)))
        loudness = loudness * jnp.repeat(draws, extent[position] // blocks).reshape([-1 if axis == position else 1 for axis in range(len(extent))])
    return loudness


def assign_block(key, own, number, rows, count, top, bound, lean):
    ranking = jax.random.permutation(key, count)
    crowded, ordinary = load_shares(count, rows * top, bound, lean, True), load_shares(count, rows * top, bound, lean, False)
    places = jnp.arange(count)

    def named(sizes, rotation):
        used = int((sizes > 0).sum())
        fixed = max(1, used // 4)
        moved = fixed + (places - fixed + rotation * (used - fixed)) % max(1, count - fixed)
        return jnp.zeros((count,), jnp.int32).at[ranking[jnp.where(places < fixed, places, moved)]].set(jnp.asarray(sizes, jnp.int32))

    sizes = jnp.where(number % 4 == 0, named(crowded, number // 4), named(ordinary, number - number // 4 - 1))
    mixed = jax.random.permutation(jax.random.fold_in(own, 3), count)
    giver, receiver = mixed[0:count // 2 * 2:2], mixed[1:count // 2 * 2:2]
    slack = jnp.minimum(sizes[giver] - 1, bound - sizes[receiver]) // 2
    slack = jnp.where((giver == ranking[0]) | (receiver == ranking[0]) | (sizes[receiver] == 0), 0, jnp.maximum(slack, 0))
    moved = jax.random.randint(jax.random.fold_in(own, 4), (count // 2,), 0, 1 << 20) % (slack + 1)
    sizes = sizes.at[giver].add(-moved).at[receiver].add(moved)
    labels = jnp.searchsorted(jnp.cumsum(sizes), jnp.arange(rows * top), side="right").astype(jnp.int32)
    listing = labels.reshape(top, rows).T
    listing = listing[jax.random.permutation(jax.random.fold_in(own, 1), rows)]
    rotation = jax.random.randint(jax.random.fold_in(own, 2), (rows, 1), 0, top)
    return jnp.take_along_axis(listing, (jnp.arange(top)[None, :] + rotation) % top, axis=1)


def load_shares(count, total, most, lean, full):
    portions = [(1 << 20) // math.isqrt(grade ** lean) + 1 for grade in range(1, count + 1)]
    largest = most if full else min(most, max(-(-total // count), total * portions[0] // sum(portions)))
    least = 1 if total - largest >= count - 1 else 0
    holding, rest = [largest] + [least] * (count - 1), total - largest - least * (count - 1)
    while rest > 0:
        candidates = [i for i in range(1, count) if holding[i] < largest] or [i for i in range(1, count) if holding[i] < most]
        mass, remaining = sum([portions[i] for i in candidates]), rest
        for i in candidates:
            more = min(most - holding[i], max(1, remaining * portions[i] // mass), rest)
            holding[i] = holding[i] + more
            rest = rest - more
    return np.array(holding)


def bell_draw(rng, extent, scale, bound, shards=(), kind=jnp.bfloat16):
    values = jax.random.normal(rng, extent, jnp.float32) * scale
    if len(shards) > 0:
        values = block_levels(rng, extent, shards, -0.22, 0.18) * values
    return jnp.clip(values, min=-bound, max=bound).astype(kind)


def setup_inputs(seed: int = 0) -> dict:
    seeds = jax.random.split(jax.random.key(seed), 18)
    tokens = draw_tokens(jax.random.fold_in(seeds[17], 71), 0)
    norm_gain = jnp.clip(1.0 + 0.18 * jax.random.normal(seeds[1], (WIDTH,), jnp.float32), 0.1, 1.9)
    post_gain = jnp.clip(1.0 + 0.18 * jax.random.normal(seeds[2], (WIDTH,), jnp.float32), 0.1, 1.9)
    w_query = bell_draw(seeds[3], (WIDTH, QUERY_HEADS * HEAD_DIM), WIDTH ** -0.5, 0.125, ((1, 8),))
    w_key = bell_draw(seeds[4], (WIDTH, KV_HEADS * HEAD_DIM), WIDTH ** -0.5, 0.125, ((1, 8),))
    w_value = bell_draw(seeds[5], (WIDTH, KV_HEADS * HEAD_DIM), WIDTH ** -0.5, 0.125, ((1, 8),))
    w_forget = bell_draw(seeds[6], (WIDTH, QUERY_HEADS), (WIDTH // 4) ** -0.5, 0.25)
    w_output = bell_draw(seeds[7], (QUERY_HEADS * HEAD_DIM, WIDTH), (QUERY_HEADS * HEAD_DIM) ** -0.5, 0.125, ((0, 8),))
    key_cache = draw_key_cache(jax.random.fold_in(seeds[17], 71), 0)
    value_cache = bell_draw(seeds[9], (SEQUENCE_TOTAL, KV_HEADS, HEAD_DIM, CACHE_POSITIONS), 1.0, 6.0, ((0, 32), (1, 8)))
    gate_cache = draw_gate_cache(jax.random.fold_in(seeds[17], 71), 0)
    lengths = with_ends(jax.random.randint(seeds[11], (SEQUENCE_TOTAL,), CACHE_POSITIONS // 4, CACHE_POSITIONS + 1), jax.random.fold_in(seeds[11], 1), CACHE_POSITIONS // 4, CACHE_POSITIONS).astype(jnp.int32)
    routes_keys = jax.random.split(jax.random.fold_in(seeds[12], 1), SEQUENCE_TOTAL // TOK_GRP)
    routes_turns = jax.random.permutation(jax.random.fold_in(seeds[12], 3), SEQUENCE_TOTAL // TOK_GRP)
    routes = jax.vmap(lambda own, number: assign_block(jax.random.fold_in(seeds[12], 2), own, number, TOK_GRP, EXPERTS, TOPK, CAP, 2))(routes_keys, routes_turns).reshape((SEQUENCE_TOTAL, TOPK))
    route_logits = bell_draw(seeds[13], (SEQUENCE_TOTAL, TOPK), 1.5, 6.0, ((0, 32),), jnp.float32)
    w_gate = bell_draw(seeds[14], (EXPERTS, WIDTH, FFN), WIDTH ** -0.5, 0.125, ((0, 32), (2, 8)))
    w_up = bell_draw(seeds[15], (EXPERTS, WIDTH, FFN), WIDTH ** -0.5, 0.125, ((0, 32), (2, 8)))
    w_down = bell_draw(seeds[16], (EXPERTS, FFN, WIDTH), FFN ** -0.5, 0.09375, ((0, 32), (1, 8)))
    return dict(tokens=tokens, norm_gain=norm_gain, post_gain=post_gain, w_query=w_query, w_key=w_key, w_value=w_value, w_forget=w_forget, w_output=w_output, key_cache=key_cache, value_cache=value_cache, gate_cache=gate_cache, lengths=lengths, routes=routes, route_logits=route_logits, w_gate=w_gate, w_up=w_up, w_down=w_down)


epsilon = 1e-06

def normalize(rows, gain):
    return rows * lax.rsqrt(lax.optimization_barrier(jnp.mean(rows * rows, axis=-1, keepdims=True)) + epsilon) * gain

def attend_one(packed):
    query_vector, fresh_key, value_new, log_forget, key_rows, value_rows, gates, length = packed
    group_size = QUERY_HEADS // KV_HEADS
    score_scale = HEAD_DIM ** (-0.5)
    grouped = query_vector.reshape(KV_HEADS, group_size, HEAD_DIM).astype(jnp.float32)
    past_scores = jnp.einsum('kgd,kdl->kgl', grouped, key_rows.astype(jnp.float32)).reshape(QUERY_HEADS, CACHE_POSITIONS)
    cache_position = jnp.arange(CACHE_POSITIONS, dtype=jnp.int32)[None, :]
    latest = lax.optimization_barrier(jnp.sum(jnp.where(cache_position == length - 1, gates, 0.0), axis=-1))
    past_scores = past_scores * score_scale + (latest + log_forget)[:, None] - gates
    past_scores = jnp.where(cache_position < length, past_scores, -jnp.inf)
    new_score = jnp.einsum('kgd,kd->kg', grouped, fresh_key.astype(jnp.float32)).reshape(QUERY_HEADS) * score_scale
    peak_score = jnp.maximum(lax.optimization_barrier(jnp.max(past_scores, axis=-1)), new_score)
    past_exp = jnp.exp(past_scores - peak_score[:, None])
    new_exp = jnp.exp(new_score - peak_score)
    denominator = lax.optimization_barrier(jnp.sum(past_exp, axis=-1)) + new_exp
    past_prob = (past_exp / denominator[:, None]).astype(jnp.bfloat16)
    new_prob = (new_exp / denominator).astype(jnp.bfloat16)
    mixed = jnp.einsum('kgl,kdl->kgd', past_prob.reshape(KV_HEADS, group_size, CACHE_POSITIONS).astype(jnp.float32), value_rows.astype(jnp.float32))
    mixed = mixed + new_prob.reshape(KV_HEADS, group_size)[:, :, None].astype(jnp.float32) * value_new[:, None, :].astype(jnp.float32)
    return mixed.reshape(QUERY_HEADS * HEAD_DIM).astype(jnp.bfloat16)

def reference(tokens, norm_gain, post_gain, w_query, w_key, w_value, w_forget, w_output, key_cache, value_cache, gate_cache, lengths, routes, route_logits, w_gate, w_up, w_down):
    tokens_wide = tokens.astype(jnp.float32)
    normed = normalize(tokens_wide, norm_gain).astype(jnp.bfloat16)
    query_vector = jnp.dot(normed, w_query, preferred_element_type=jnp.float32).astype(jnp.bfloat16)
    fresh_key = jnp.dot(normed, w_key, preferred_element_type=jnp.float32).astype(jnp.bfloat16)
    value_new = jnp.dot(normed, w_value, preferred_element_type=jnp.float32).astype(jnp.bfloat16)
    log_forget = jax.nn.log_sigmoid(jnp.dot(normed, w_forget, preferred_element_type=jnp.float32))
    attended = lax.map(attend_one, (query_vector, fresh_key.reshape(SEQUENCE_TOTAL, KV_HEADS, HEAD_DIM), value_new.reshape(SEQUENCE_TOTAL, KV_HEADS, HEAD_DIM), log_forget, key_cache, value_cache, gate_cache, lengths))
    head_block = QUERY_HEADS * HEAD_DIM // N_TP
    blocks = attended.reshape(SEQUENCE_TOTAL, N_TP, head_block).transpose(1, 0, 2).astype(jnp.float32)
    parts = jnp.einsum('tsr,trw->tsw', blocks, w_output.reshape(N_TP, head_block, WIDTH).astype(jnp.float32))
    attention = lax.optimization_barrier(jnp.sum(parts.astype(jnp.bfloat16).astype(jnp.float32), axis=0))
    stream = tokens_wide + attention
    expert_input = normalize(stream, post_gain).astype(jnp.bfloat16)
    route_count = SEQUENCE_TOTAL * TOPK
    per_expert = CAP * N_EP
    flat_routes = routes.reshape(route_count)
    expert_onehot = (flat_routes[:, None] == jnp.arange(EXPERTS, dtype=jnp.int32)[None, :]).astype(jnp.int32)
    route_rank = lax.optimization_barrier(jnp.sum(jnp.cumsum(expert_onehot, axis=0) * expert_onehot, axis=1)) - 1
    slot_index = (flat_routes * per_expert + route_rank).astype(jnp.int32)
    slot_token = jnp.zeros((EXPERTS * per_expert,), jnp.int32).at[slot_index].set(jnp.arange(route_count, dtype=jnp.int32) // TOPK)
    ff_block = FFN // N_TP

    def run_expert(index):
        chosen = lax.dynamic_slice_in_dim(slot_token, (index * per_expert).astype(jnp.int32), per_expert)
        expert_rows = expert_input[chosen]
        gate_act = jnp.dot(expert_rows, w_gate[index], preferred_element_type=jnp.float32)
        upper = jnp.dot(expert_rows, w_up[index], preferred_element_type=jnp.float32)
        hidden_act = (jax.nn.silu(gate_act) * upper).astype(jnp.bfloat16)
        down_parts = jnp.einsum('rtf,tfw->trw', hidden_act.reshape(per_expert, N_TP, ff_block).astype(jnp.float32), w_down[index].reshape(N_TP, ff_block, WIDTH).astype(jnp.float32))
        return lax.optimization_barrier(jnp.sum(down_parts.astype(jnp.bfloat16).astype(jnp.float32), axis=0)).astype(jnp.bfloat16)
    outputs = lax.map(run_expert, jnp.arange(EXPERTS, dtype=jnp.int32))
    picked = outputs.reshape(EXPERTS * per_expert, WIDTH)[slot_index].astype(jnp.float32).reshape(SEQUENCE_TOTAL, TOPK, WIDTH)
    route_weight = jax.nn.softmax(route_logits, axis=-1)
    expert_mix = lax.optimization_barrier(jnp.sum(route_weight[:, :, None] * picked, axis=1))
    return (stream + expert_mix).astype(jnp.bfloat16)
```

```python
import functools

import jax
import jax.numpy as jnp
from jax import lax
from jax.experimental import pallas as pl
from jax.experimental.pallas import tpu as pltpu
from jax.sharding import PartitionSpec as P

f32 = jnp.float32
bf16 = jnp.bfloat16
MESH = pl.DeviceIdType.MESH
EPSILON = 1e-06


def mm(a, b):
    return jnp.dot(a, b, preferred_element_type=f32)


def mm_nt(a, b):
    return lax.dot_general(a, b, (((1,), (1,)), ((), ())), preferred_element_type=f32)


def iota(shape, dim):
    return lax.broadcasted_iota(jnp.int32, shape, dim)


def interleave(even, odd):
    low = iota(even.shape, 1) < 4
    first = jnp.where(low, even, pltpu.roll(odd, 4, 1))
    second = jnp.where(low, pltpu.roll(even, 4, 1), odd)
    return first, second


def kernel(n_ep, n_tp, *refs):
    hbm = refs[:17]
    out_ref = refs[17]
    (
        tok, ngain, pgain, wq, wk, wv, wf, wo, keys, vals, gates, lens, routes, logits, wg, wu, wd,
    ) = refs[18:35]
    (
        probs, asend, arecv, packed, arrived, blocks, psend, precv, tsend, trecv, ret_send, ret,
        load_sem, a_s, a_r, d_s, d_r, g_s, g_r, p_s, p_r, t_s, t_r, b_s, b_r,
    ) = refs[35:]
    n_y = n_tp // 2
    me = lax.axis_index("ep")
    t = lax.axis_index("tp")
    y = t // 2
    c = t % 2
    seqs, width = tok.shape
    heads = gates.shape[1]
    rows = seqs * heads
    span = keys.shape[1]
    hd = keys.shape[0] // seqs
    own = width // n_tp

    def tp_at(dy, dc):
        return ((y + dy) % n_y) * 2 + (c if dc == 0 else 1 - c)

    def tp_from(dy, dc):
        return ((y + n_y - dy) % n_y) * 2 + (c if dc == 0 else 1 - c)

    def load(n, dst, part=None):
        src = hbm[n]
        if part is not None:
            src, dst = src.at[part], dst.at[part]
        load.count += 1
        copy = pltpu.make_async_copy(src, dst, load_sem.at[load.count - 1])
        copy.start()
        return copy

    load.count = 0
    group = 4
    n_groups = seqs // group
    gr = group * heads
    gk = group * hd
    chunk = 2
    slices = [pl.ds(n * chunk * gk, chunk * gk) for n in range(n_groups // chunk)]
    l_tok = load(0, tok)
    l_ngain = load(1, ngain)
    l_wq = load(3, wq)
    l_wk = load(4, wk)
    l_wv = load(5, wv)
    l_wf = load(6, wf)
    l_small = [load(11, lens), load(12, routes), load(13, logits), load(2, pgain)]
    l_keys = [load(8, keys, s) for s in slices]
    l_gates = load(10, gates)
    l_vals = [load(9, vals, s) for s in slices]
    l_wo = load(7, wo)
    l_wg = load(14, wg)
    l_wu = load(15, wu)
    l_wd = load(16, wd)

    barrier = pltpu.get_barrier_semaphore()
    for k in range(1, n_ep):
        pl.semaphore_signal(
            barrier, inc=1, device_id={"ep": (me + k) % n_ep}, device_id_type=MESH
        )
    for n in range(1, n_tp):
        pl.semaphore_signal(
            barrier, inc=1, device_id={"tp": tp_at(n // 2, n % 2)}, device_id_type=MESH
        )

    l_tok.wait()
    l_ngain.wait()
    x = tok[...].astype(f32)
    normed = x * lax.rsqrt(jnp.mean(x * x, axis=-1, keepdims=True) + EPSILON) * ngain[...]
    repeat = (iota((rows, seqs), 0) // heads) == iota((rows, seqs), 1)
    normed = mm(repeat.astype(bf16), normed.astype(bf16)).astype(bf16)
    l_wq.wait()
    q = mm(normed, wq[...]).astype(bf16).astype(f32)
    l_wk.wait()
    k_new = mm_nt(normed, wk[...]).astype(bf16).astype(f32)
    l_wv.wait()
    v_new = mm_nt(normed, wv[...]).astype(bf16).astype(f32)
    l_wf.wait()
    forget = mm_nt(normed, wf[...])
    for copy in l_small:
        copy.wait()

    row = iota((rows, heads * hd), 0)
    block = iota((rows, heads * hd), 1) // hd
    q = jnp.where(block == row % heads, q, 0.0)
    half = heads * hd // 2
    q = q[:, :half] + q[:, half:]
    q = q + pltpu.roll(q, hd, 1)
    new_score = jnp.sum(q[:, :hd] * k_new, axis=1, keepdims=True) * hd**-0.5
    diagonal = block == (row // heads) % group
    q = jnp.where(diagonal, jnp.concatenate([q, q], axis=1) * hd**-0.5, 0.0).astype(bf16)
    head_row = iota(forget.shape, 0) % heads
    picked = iota(forget.shape, 1) == t * heads + head_row
    forget = jnp.sum(jnp.where(picked, forget, 0.0), axis=1, keepdims=True)
    log_forget = jnp.minimum(forget, 0.0) - jnp.log1p(jnp.exp(-jnp.abs(forget)))
    length = jnp.sum(
        jnp.where(repeat, lens[...].astype(f32), 0.0), axis=1, keepdims=True
    ).astype(jnp.int32)

    new_probs = []
    l_gates.wait()
    for g in range(n_groups):
        if g % chunk == 0:
            l_keys[g // chunk].wait()
        at = slice(g * gr, (g + 1) * gr)
        score = mm(q[at], keys[pl.ds(g * gk, gk), :])
        gate = jnp.concatenate([gates[g * group + n] for n in range(group)], axis=0)
        position = iota((gr, span), 1)
        latest = jnp.sum(
            jnp.where(position == length[at] - 1, gate, 0.0), axis=1, keepdims=True
        )
        score = score + (latest + log_forget[at]) - gate
        score = jnp.where(position < length[at], score, -jnp.inf)
        peak = jnp.maximum(jnp.max(score, axis=1, keepdims=True), new_score[at])
        past = jnp.exp(score - peak)
        new = jnp.exp(new_score[at] - peak)
        scale = 1.0 / (jnp.sum(past, axis=1, keepdims=True) + new)
        probs[pl.ds(g * gr, gr), :] = (past * scale).astype(bf16)
        new_probs.append((new * scale).astype(bf16).astype(f32))
    mixed = []
    for g in range(n_groups):
        if g % chunk == 0:
            l_vals[g // chunk].wait()
        mixed.append(mm_nt(probs[pl.ds(g * gr, gr), :], vals[pl.ds(g * gk, gk), :]))
    mixed = jnp.where(diagonal, jnp.concatenate(mixed, axis=0), 0.0)
    mixed = mixed[:, :half] + mixed[:, half:]
    mixed = mixed + pltpu.roll(mixed, hd, 1)
    mixed = mixed[:, :hd] + jnp.concatenate(new_probs, axis=0) * v_new
    spread = (iota((hd, heads * hd), 1) % hd) == iota((hd, heads * hd), 0)
    mixed = mm(mixed.astype(bf16), spread.astype(bf16))
    mixed = jnp.where(block == row % heads, mixed, 0.0).astype(bf16)
    gather = (iota((seqs, rows), 1) // heads) == iota((seqs, rows), 0)
    attended = mm(gather.astype(bf16), mixed).astype(bf16)

    l_wo.wait()
    pl.semaphore_wait(barrier, n_ep - 1 + n_tp - 1)
    copies = []
    order = [4, 5, 2, 6, 3, 7, 1]
    for n in order:
        to = tp_at(n // 2, n % 2)
        asend[n] = mm(attended, wo[:, pl.ds(pl.multiple_of(to * own, own), own)]).astype(bf16)
        copy = pltpu.make_async_remote_copy(
            asend.at[n], arecv.at[n], a_s.at[n], a_r.at[n],
            device_id={"tp": to}, device_id_type=MESH,
        )
        copy.start()
        copies.append(copy)
    own_cols = pl.ds(pl.multiple_of(t * own, own), own)
    stream = tok[:, own_cols].astype(f32)
    stream = stream + mm(attended, wo[:, own_cols]).astype(bf16).astype(f32)

    cols = 8 * n_ep
    lanes = own // 2
    q_at = iota((seqs, cols), 1)
    expert = (me + q_at // 8) % n_ep
    eye = iota((seqs, seqs), 0) == iota((seqs, seqs), 1)

    def column(ref, n):
        return jnp.sum(jnp.where(eye, ref[n : n + 1, :].astype(f32), 0.0), axis=1, keepdims=True)

    first = column(routes, 0).astype(jnp.int32) == expert
    second = column(routes, 1).astype(jnp.int32) == expert
    named = jnp.logical_or(first, second)
    before = iota((seqs, seqs), 1) < iota((seqs, seqs), 0)
    rank = mm(before.astype(bf16), named.astype(bf16))
    taken = jnp.logical_and(named, rank == (q_at % 4).astype(f32))
    l0, l1 = column(logits, 0), column(logits, 1)
    peak = jnp.maximum(l0, l1)
    e0 = jnp.exp(l0 - peak)
    e1 = jnp.exp(l1 - peak)
    weight = jnp.where(first, e0 / (e0 + e1), e1 / (e0 + e1))
    left = (q_at // 4) % 2 == 0
    slots = jnp.where(taken, 1.0, 0.0)
    slots = jnp.concatenate([jnp.where(left, slots, 0.0), jnp.where(left, 0.0, slots)], axis=0)
    combine = slots * jnp.concatenate([weight, weight], axis=0)
    dispatch = jnp.transpose(slots).astype(bf16)

    for copy in copies:
        copy.wait_recv()
    for n in order:
        stream = stream + arecv[n].astype(f32)

    sent = stream.astype(bf16)
    sent = jnp.concatenate([sent[:, :lanes], sent[:, lanes:]], axis=0)
    packed[...] = mm(dispatch, sent).astype(bf16).reshape(n_ep, 8, lanes)
    far = sorted(range(1, n_ep), key=lambda k: -(min(k // 4, 8 - k // 4) + min(k % 4, 4 - k % 4)))
    for k in far:
        pltpu.make_async_remote_copy(
            packed.at[k], arrived.at[k], d_s, d_r,
            device_id={"ep": (me + k) % n_ep}, device_id_type=MESH,
        ).start()
    arrived[0] = packed[0]
    rest = pl.ds(1, n_ep - 1)
    dispatched = pltpu.make_async_remote_copy(
        packed.at[rest], arrived.at[rest], d_s, d_r,
        device_id={"ep": (me + 1) % n_ep}, device_id_type=MESH,
    )
    dispatched.wait_recv()

    got = arrived[...].astype(f32).reshape(n_ep // 2, 2, 8, lanes)
    lo, hi = interleave(got[:, 0], got[:, 1])
    slot_rows = 4 * n_ep
    blocks[0] = jnp.concatenate(
        [lo.reshape(slot_rows, lanes), hi.reshape(slot_rows, lanes)], axis=1
    ).astype(bf16)
    g_copies = {}

    def gather_send(src, dst, to):
        copy = pltpu.make_async_remote_copy(
            blocks.at[src], blocks.at[dst], g_s.at[dst], g_r.at[dst],
            device_id={"tp": to}, device_id_type=MESH,
        )
        copy.start()
        g_copies[dst] = copy

    for dy in (2, 1, 3):
        gather_send(0, 2 * dy, tp_at(dy, 0))
    gather_send(0, 1, tp_at(0, 1))
    l_wg.wait()
    l_wu.wait()
    gate_act = upper = squares = None
    for n in (0, 1, 2, 6, 3, 7, 4, 5):
        if n:
            g_copies[n].wait_recv()
        if n in (2, 6, 4):
            gather_send(n, n + 1, tp_at(0, 1))
        cols_n = pl.ds(pl.multiple_of(tp_from(n // 2, n % 2) * own, own), own)
        part = blocks[n].astype(f32)
        square = jnp.sum(part * part, axis=1, keepdims=True)
        part = (part * pgain[:, cols_n]).astype(bf16)
        gate_part = mm_nt(part, wg[:, cols_n])
        upper_part = mm_nt(part, wu[:, cols_n])
        gate_act = gate_part if n == 0 else gate_act + gate_part
        upper = upper_part if n == 0 else upper + upper_part
        squares = square if n == 0 else squares + square
    norm = lax.rsqrt(squares / width + EPSILON)
    gate_act = gate_act * norm
    hidden = ((gate_act / (1.0 + jnp.exp(-gate_act))) * (upper * norm)).astype(bf16)

    l_wd.wait()

    def down(dy, dc):
        at = pl.ds(pl.multiple_of(tp_at(dy, dc) * own, own), own)
        return mm(hidden, wd[:, at])

    p_copies = {}
    for dy in (2, 1, 3, 0):
        psend[dy] = down(dy, 1).astype(bf16)
        copy = pltpu.make_async_remote_copy(
            psend.at[dy], precv.at[dy], p_s.at[dy], p_r.at[dy],
            device_id={"tp": tp_at(0, 1)}, device_id_type=MESH,
        )
        copy.start()
        p_copies[dy] = copy
    t_copies = {}
    for dy in (2, 1, 3, 0):
        part = down(dy, 0)
        p_copies[dy].wait_recv()
        part = part + precv[dy].astype(f32)
        if dy == 0:
            total = part
        else:
            tsend[dy] = part.astype(bf16)
            copy = pltpu.make_async_remote_copy(
                tsend.at[dy], trecv.at[dy], t_s.at[dy], t_r.at[dy],
                device_id={"tp": tp_at(dy, 0)}, device_id_type=MESH,
            )
            copy.start()
            t_copies[dy] = copy
    for dy in (1, 3, 2):
        t_copies[dy].wait_recv()
        total = total + trecv[dy].astype(f32)

    lo, hi = interleave(
        total[:, :lanes].reshape(n_ep // 2, 8, lanes), total[:, lanes:].reshape(n_ep // 2, 8, lanes)
    )
    ret_send[...] = jnp.stack([lo, hi], axis=1).reshape(n_ep, 8, lanes).astype(bf16)
    for k in far:
        pltpu.make_async_remote_copy(
            ret_send.at[k], ret.at[k], b_s, b_r,
            device_id={"ep": (me + n_ep - k) % n_ep}, device_id_type=MESH,
        ).start()
    ret[0] = ret_send[0]
    high = combine.astype(bf16)
    left_over = combine - high.astype(f32)
    mid = left_over.astype(bf16)
    low = (left_over - mid.astype(f32)).astype(bf16)
    returned = pltpu.make_async_remote_copy(
        ret_send.at[rest], ret.at[rest], b_s, b_r,
        device_id={"ep": (me + n_ep - 1) % n_ep}, device_id_type=MESH,
    )
    returned.wait_recv()
    back = ret[...].reshape(cols, lanes)
    mix = mm(high, back) + mm(mid, back) + mm(low, back)
    out_ref[:, :lanes] = (stream[:, :lanes] + mix[:seqs]).astype(bf16)
    out_ref[:, lanes:] = (stream[:, lanes:] + mix[seqs:]).astype(bf16)

    for copy in copies:
        copy.wait_send()
    dispatched.wait_send()
    for some in (g_copies, p_copies, t_copies):
        for copy in some.values():
            copy.wait_send()
    returned.wait_send()


def body(n_ep, n_tp, *args):
    (
        tokens, norm_gain, post_gain, w_query, w_key, w_value, w_forget, w_output,
        key_cache, value_cache, gate_cache, lengths, routes, route_logits, w_gate, w_up, w_down,
    ) = args
    seqs, width = tokens.shape
    hd, span = key_cache.shape[2:]
    heads = gate_cache.shape[1]
    own = width // n_tp
    operands = (
        tokens, norm_gain.reshape(1, width), post_gain.reshape(1, width),
        w_query, w_key.T, w_value.T, w_forget.T, w_output,
        key_cache.reshape(seqs * hd, span), value_cache.reshape(seqs * hd, span), gate_cache,
        lengths.reshape(1, seqs), routes.T, route_logits.T, w_gate[0].T, w_up[0].T, w_down[0],
    )
    slots = 4 * n_ep
    dma = pltpu.SemaphoreType.DMA
    scratch = [pltpu.VMEM(a.shape, a.dtype) for a in operands] + [
        pltpu.VMEM((seqs * heads, span), bf16),
        pltpu.VMEM((n_tp, seqs, own), bf16),
        pltpu.VMEM((n_tp, seqs, own), bf16),
        pltpu.VMEM((n_ep, 8, own // 2), bf16),
        pltpu.VMEM((n_ep, 8, own // 2), bf16),
        pltpu.VMEM((n_tp, slots, own), bf16),
        pltpu.VMEM((n_tp // 2, slots, own), bf16),
        pltpu.VMEM((n_tp // 2, slots, own), bf16),
        pltpu.VMEM((n_tp // 2, slots, own), bf16),
        pltpu.VMEM((n_tp // 2, slots, own), bf16),
        pltpu.VMEM((n_ep, 8, own // 2), bf16),
        pltpu.VMEM((n_ep, 8, own // 2), bf16),
        dma((32,)),
        dma((n_tp,)), dma((n_tp,)),
        dma, dma,
        dma((n_tp,)), dma((n_tp,)),
        dma((n_tp // 2,)), dma((n_tp // 2,)),
        dma((n_tp // 2,)), dma((n_tp // 2,)),
        dma, dma,
    ]
    return pl.pallas_call(
        functools.partial(kernel, n_ep, n_tp),
        out_shape=jax.ShapeDtypeStruct((seqs, own), bf16),
        in_specs=[pl.BlockSpec(memory_space=pl.ANY)] * len(operands),
        out_specs=pl.BlockSpec(memory_space=pltpu.VMEM),
        scratch_shapes=scratch,
        compiler_params=pltpu.CompilerParams(
            collective_id=0, has_side_effects=True, vmem_limit_bytes=60 * 1024 * 1024
        ),
        name="layer",
    )(*operands)


def solution(mesh):
    in_specs = (
        P("ep", None),
        P(),
        P(),
        P(None, "tp"),
        P(None, "tp"),
        P(None, "tp"),
        P(),
        P("tp", None),
        P("ep", "tp", None, None),
        P("ep", "tp", None, None),
        P("ep", "tp", None),
        P("ep"),
        P("ep", None),
        P("ep", None),
        P("ep", None, "tp"),
        P("ep", None, "tp"),
        P("ep", "tp", None),
    )
    step = functools.partial(body, mesh.shape["ep"], mesh.shape["tp"])
    return jax.shard_map(
        step, mesh=mesh, in_specs=in_specs, out_specs=P("ep", "tp"), check_vma=False
    )
```

```python
import functools

import jax
import jax.numpy as jnp
from jax import lax
from jax.experimental import pallas as pl
from jax.experimental.pallas import tpu as pltpu
from jax.sharding import PartitionSpec as P

f32 = jnp.float32
bf16 = jnp.bfloat16
MESH = pl.DeviceIdType.MESH
EPSILON = 1e-06
NX = 4


def mm(a, b):
    return jnp.dot(a, b, preferred_element_type=f32)


def mm_nt(a, b):
    return lax.dot_general(a, b, (((1,), (1,)), ((), ())), preferred_element_type=f32)


def iota(shape, dim):
    return lax.broadcasted_iota(jnp.int32, shape, dim)


def interleave(even, odd):
    low = iota(even.shape, 1) < 4
    first = jnp.where(low, even, pltpu.roll(odd, 4, 1))
    second = jnp.where(low, pltpu.roll(even, 4, 1), odd)
    return first, second


def kernel(n_ep, n_tp, *refs):
    hbm = refs[:17]
    out_ref = refs[17]
    (
        tok, ngain, pgain, wq, wkvf, wo, keys, vals, gates, lens, routes, logits, wg, wu, wd,
    ) = refs[18:33]
    (
        probs, asend, arecv, packed, arrived, blocks, psend, precv, tsend, trecv, ret_send, ret,
        load_sem, a_s, a_r, d_s, d_r, g_s, g_r, p_s, p_r, t_s, t_r, b_s, b_r,
    ) = refs[33:]
    n_y = n_tp // 2
    me = lax.axis_index("ep")
    t = lax.axis_index("tp")
    y = t // 2
    c = t % 2
    seqs, width = tok.shape
    heads = gates.shape[1]
    rows = seqs * heads
    span = keys.shape[1]
    hd = keys.shape[0] // seqs
    own = width // n_tp

    n_z = n_ep // NX
    z = me // NX
    xx = me % NX
    near = 5 * NX
    offsets = [(kz, kx) for kz in (0, 1, 2, 6, 7, 3, 4, 5) for kx in range(NX)]

    def ep_at(p, sign=1):
        kz, kx = offsets[p]
        if sign < 0:
            kz, kx = n_z - kz, NX - kx
        return ((z + kz) % n_z) * NX + (xx + kx) % NX

    def tp_at(dy, dc):
        return ((y + dy) % n_y) * 2 + (c if dc == 0 else 1 - c)

    def tp_from(dy, dc):
        return ((y + n_y - dy) % n_y) * 2 + (c if dc == 0 else 1 - c)

    def load(n, dst, part=None, into=None):
        src = hbm[n]
        if part is not None:
            src, dst = src.at[part], dst.at[part]
        if into is not None:
            dst = dst.at[pl.ds(into, src.shape[0])]
        load.count += 1
        copy = pltpu.make_async_copy(src, dst, load_sem.at[load.count - 1])
        copy.start()
        return copy

    load.count = 0
    group = 4
    n_groups = seqs // group
    gr = group * heads
    gk = group * hd
    chunk = 2
    slices = [pl.ds(n * chunk * gk, chunk * gk) for n in range(n_groups // chunk)]
    l_tok = load(0, tok)
    l_ngain = load(1, ngain)
    l_wq = load(3, wq)
    l_kvf = [load(4, wkvf, into=0), load(5, wkvf, into=hd), load(6, wkvf, into=2 * hd)]
    l_small = [load(11, lens), load(12, routes), load(13, logits), load(2, pgain)]
    l_gates = load(10, gates)
    l_keys, l_vals = [], []
    for s in slices:
        l_keys.append(load(8, keys, s))
        l_vals.append(load(9, vals, s))
    l_wo = load(7, wo)
    l_wg = load(14, wg)
    l_wu = load(15, wu)
    l_wd = load(16, wd)

    barrier = pltpu.get_barrier_semaphore()
    for k in range(1, n_ep):
        pl.semaphore_signal(
            barrier, inc=1, device_id={"ep": ep_at(k)}, device_id_type=MESH
        )
    for n in range(1, n_tp):
        pl.semaphore_signal(
            barrier, inc=1, device_id={"tp": tp_at(n // 2, n % 2)}, device_id_type=MESH
        )

    l_tok.wait()
    l_ngain.wait()
    x = tok[...].astype(f32)
    normed = x * lax.rsqrt(jnp.mean(x * x, axis=-1, keepdims=True) + EPSILON) * ngain[...]
    repeat = (iota((rows, seqs), 0) // heads) == iota((rows, seqs), 1)
    normed = mm(repeat.astype(bf16), normed.astype(bf16)).astype(bf16)
    l_wq.wait()
    q = mm(normed, wq[...]).astype(bf16).astype(f32)
    for copy in l_kvf:
        copy.wait()
    kvf = mm_nt(normed, wkvf[...])
    k_new = kvf[:, :hd].astype(bf16).astype(f32)
    v_new = kvf[:, hd : 2 * hd].astype(bf16).astype(f32)
    forget = kvf[:, 2 * hd :]
    for copy in l_small:
        copy.wait()

    row = iota((rows, heads * hd), 0)
    block = iota((rows, heads * hd), 1) // hd
    q = jnp.where(block == row % heads, q, 0.0)
    half = heads * hd // 2
    q = q[:, :half] + q[:, half:]
    q = q + pltpu.roll(q, hd, 1)
    new_score = jnp.sum(q[:, :hd] * k_new, axis=1, keepdims=True) * hd**-0.5
    diagonal = block == (row // heads) % group
    q = jnp.where(diagonal, jnp.concatenate([q, q], axis=1) * hd**-0.5, 0.0).astype(bf16)
    head_row = iota(forget.shape, 0) % heads
    picked = iota(forget.shape, 1) == t * heads + head_row
    forget = jnp.sum(jnp.where(picked, forget, 0.0), axis=1, keepdims=True)
    log_forget = jnp.minimum(forget, 0.0) - jnp.log1p(jnp.exp(-jnp.abs(forget)))
    length = jnp.sum(
        jnp.where(repeat, lens[...].astype(f32), 0.0), axis=1, keepdims=True
    ).astype(jnp.int32)

    new_probs, mixed = [], []
    l_gates.wait()

    def weigh(g):
        mixed.append(mm_nt(probs[pl.ds(g * gr, gr), :], vals[pl.ds(g * gk, gk), :]))

    for g in range(n_groups):
        if g % chunk == 0:
            l_keys[g // chunk].wait()
        at = slice(g * gr, (g + 1) * gr)
        score = mm(q[at], keys[pl.ds(g * gk, gk), :])
        if g >= chunk:
            if g % chunk == 0:
                l_vals[g // chunk - 1].wait()
            weigh(g - chunk)
        gate = jnp.concatenate([gates[g * group + n] for n in range(group)], axis=0)
        position = iota((gr, span), 1)
        latest = jnp.sum(
            jnp.where(position == length[at] - 1, gate, 0.0), axis=1, keepdims=True
        )
        score = score + (latest + log_forget[at]) - gate
        score = jnp.where(position < length[at], score, -jnp.inf)
        peak = jnp.maximum(jnp.max(score, axis=1, keepdims=True), new_score[at])
        past = jnp.exp(score - peak)
        new = jnp.exp(new_score[at] - peak)
        scale = 1.0 / (jnp.sum(past, axis=1, keepdims=True) + new)
        probs[pl.ds(g * gr, gr), :] = (past * scale).astype(bf16)
        new_probs.append((new * scale).astype(bf16).astype(f32))
    l_vals[-1].wait()
    for g in range(n_groups - chunk, n_groups):
        weigh(g)
    mixed = jnp.where(diagonal, jnp.concatenate(mixed, axis=0), 0.0)
    mixed = mixed[:, :half] + mixed[:, half:]
    mixed = mixed + pltpu.roll(mixed, hd, 1)
    mixed = mixed[:, :hd] + jnp.concatenate(new_probs, axis=0) * v_new
    spread = (iota((hd, heads * hd), 1) % hd) == iota((hd, heads * hd), 0)
    mixed = mm(mixed.astype(bf16), spread.astype(bf16))
    mixed = jnp.where(block == row % heads, mixed, 0.0).astype(bf16)
    gather = (iota((seqs, rows), 1) // heads) == iota((seqs, rows), 0)
    attended = mm(gather.astype(bf16), mixed).astype(bf16)

    l_wo.wait()
    partial = mm(attended, wo[...]).astype(bf16)
    for n in range(n_tp):
        asend[n] = partial[:, n * own : (n + 1) * own]
    pl.semaphore_wait(barrier, n_ep - 1 + n_tp - 1)
    copies = []
    order = [4, 5, 2, 6, 3, 7, 1]
    for n in order:
        to = tp_at(n // 2, n % 2)
        copy = pltpu.make_async_remote_copy(
            asend.at[to], arecv.at[n], a_s.at[n], a_r.at[n],
            device_id={"tp": to}, device_id_type=MESH,
        )
        copy.start()
        copies.append(copy)
    own_cols = pl.ds(pl.multiple_of(t * own, own), own)
    stream = tok[:, own_cols].astype(f32) + asend[t].astype(f32)

    cols = 8 * n_ep
    lanes = own // 2
    q_at = iota((seqs, cols), 1)
    pz = q_at >> 5
    pz = jnp.where(pz < 3, pz, jnp.where(pz < 5, pz + 3, pz - 2))
    expert = ((z + pz) & (n_z - 1)) * NX + ((xx + (q_at >> 3)) & (NX - 1))
    eye = iota((seqs, seqs), 0) == iota((seqs, seqs), 1)

    def column(ref, n):
        return jnp.sum(jnp.where(eye, ref[n : n + 1, :].astype(f32), 0.0), axis=1, keepdims=True)

    first = column(routes, 0).astype(jnp.int32) == expert
    second = column(routes, 1).astype(jnp.int32) == expert
    named = jnp.logical_or(first, second)
    before = iota((seqs, seqs), 1) < iota((seqs, seqs), 0)
    rank = mm(before.astype(bf16), named.astype(bf16))
    taken = jnp.logical_and(named, rank == (q_at & 3).astype(f32))
    l0, l1 = column(logits, 0), column(logits, 1)
    peak = jnp.maximum(l0, l1)
    e0 = jnp.exp(l0 - peak)
    e1 = jnp.exp(l1 - peak)
    weight = jnp.where(first, e0 / (e0 + e1), e1 / (e0 + e1))
    left = (q_at & 4) == 0
    slots = jnp.where(taken, 1.0, 0.0)
    slots = jnp.concatenate([jnp.where(left, slots, 0.0), jnp.where(left, 0.0, slots)], axis=0)
    combine = slots * jnp.concatenate([weight, weight], axis=0)
    dispatch = jnp.transpose(slots).astype(bf16)

    for copy in copies:
        copy.wait_recv()
    for n in order:
        stream = stream + arecv[n].astype(f32)

    sent = stream.astype(bf16)
    sent = jnp.concatenate([sent[:, :lanes], sent[:, lanes:]], axis=0)
    packed[...] = mm(dispatch, sent).astype(bf16).reshape(n_ep, 8, lanes)
    spans = [range(1, near), range(near, n_ep)]

    def over_ep(src, dst, send, recv, part, sign):
        for p in reversed(spans[part]):
            pltpu.make_async_remote_copy(
                src.at[p], dst.at[p], send.at[part], recv.at[part],
                device_id={"ep": ep_at(p, sign)}, device_id_type=MESH,
            ).start()
        at = pl.ds(spans[part][0], len(spans[part]))
        return pltpu.make_async_remote_copy(
            src.at[at], dst.at[at], send.at[part], recv.at[part],
            device_id={"ep": ep_at(1, sign)}, device_id_type=MESH,
        )

    FAR, NEAR = 1, 0
    dispatched = {part: over_ep(packed, arrived, d_s, d_r, part, 1) for part in (FAR, NEAR)}
    arrived[0] = packed[0]

    first_block = [0, near]
    block_count = [near, n_ep - near]
    row_span = [pl.ds(4 * first_block[part], 4 * block_count[part]) for part in (NEAR, FAR)]
    g_copies = {}

    def gather_send(part, src, dst, to):
        copy = pltpu.make_async_remote_copy(
            blocks.at[src, row_span[part]], blocks.at[dst, row_span[part]],
            g_s.at[part, dst], g_r.at[part, dst],
            device_id={"tp": to}, device_id_type=MESH,
        )
        copy.start()
        g_copies[part, dst] = copy

    def take(part):
        dispatched[part].wait_recv()
        count = block_count[part]
        got = arrived[pl.ds(first_block[part], count)].astype(f32)
        got = got.reshape(count // 2, 2, 8, lanes)
        lo, hi = interleave(got[:, 0], got[:, 1])
        blocks[0, row_span[part], :] = jnp.concatenate(
            [lo.reshape(4 * count, lanes), hi.reshape(4 * count, lanes)], axis=1
        ).astype(bf16)
        for dy in (2, 1, 3):
            gather_send(part, 0, 2 * dy, tp_at(dy, 0))
        gather_send(part, 0, 1, tp_at(0, 1))

    take(NEAR)
    take(FAR)
    l_wg.wait()
    l_wu.wait()
    sums = [None, None, None]

    def expand(n):
        cols_n = pl.ds(pl.multiple_of(tp_from(n // 2, n % 2) * own, own), own)
        part = blocks[n].astype(f32)
        square = jnp.sum(part * part, axis=1, keepdims=True)
        part = (part * pgain[:, cols_n]).astype(bf16)
        for at, add in enumerate((mm_nt(part, wg[:, cols_n]), mm_nt(part, wu[:, cols_n]), square)):
            sums[at] = add if sums[at] is None else sums[at] + add

    def hear(part, n):
        g_copies[part, n].wait_recv()
        if n in (2, 4, 6):
            gather_send(part, n, n + 1, tp_at(0, 1))

    for n in (1, 2, 6):
        hear(NEAR, n)
    expand(0)
    hear(FAR, 1)
    expand(1)
    hear(NEAR, 4)
    hear(FAR, 2)
    hear(NEAR, 3)
    expand(2)
    hear(FAR, 6)
    hear(NEAR, 7)
    expand(6)
    hear(FAR, 4)
    hear(NEAR, 5)
    for n in (3, 7, 4, 5):
        if n != 4:
            hear(FAR, n)
        expand(n)
    gate_act, upper, squares = sums
    norm = lax.rsqrt(squares / width + EPSILON)
    gate_act = gate_act * norm
    hidden = ((gate_act / (1.0 + jnp.exp(-gate_act))) * (upper * norm)).astype(bf16)

    l_wd.wait()

    def down(dy, dc):
        at = pl.ds(pl.multiple_of(tp_at(dy, dc) * own, own), own)
        return mm(hidden, wd[:, at])

    p_copies = {}
    for some in ((2,), (1, 3, 0)):
        for dy in some:
            psend[dy] = down(dy, 1).astype(bf16)
        for dy in some:
            p_copies[dy] = pltpu.make_async_remote_copy(
                psend.at[dy], precv.at[dy], p_s.at[dy], p_r.at[dy],
                device_id={"tp": tp_at(0, 1)}, device_id_type=MESH,
            )
            p_copies[dy].start()
    parts = {dy: down(dy, 0) for dy in (2, 1, 3, 0)}
    t_copies = {}

    def along_y(part, dy):
        at = row_span[part]
        t_copies[part, dy] = pltpu.make_async_remote_copy(
            tsend.at[dy, at], trecv.at[dy, at], t_s.at[part, dy], t_r.at[part, dy],
            device_id={"tp": tp_at(dy, 0)}, device_id_type=MESH,
        )
        t_copies[part, dy].start()

    for dy in (2, 1, 3):
        p_copies[dy].wait_recv()
        tsend[dy] = (parts[dy] + precv[dy].astype(f32)).astype(bf16)
        along_y(FAR, dy)
    for dy in (2, 1, 3):
        along_y(NEAR, dy)
    p_copies[0].wait_recv()
    total = parts[0] + precv[0].astype(f32)

    returned = {}

    def give_back(part):
        for dy in (1, 3, 2):
            t_copies[part, dy].wait_recv()
        count = block_count[part]
        rows_at = slice(4 * first_block[part], 4 * (first_block[part] + count))
        mine = total[rows_at]
        for dy in (1, 3, 2):
            mine = mine + trecv[dy, row_span[part], :].astype(f32)
        lo, hi = interleave(
            mine[:, :lanes].reshape(count // 2, 8, lanes), mine[:, lanes:].reshape(count // 2, 8, lanes)
        )
        ret_send[pl.ds(first_block[part], count)] = (
            jnp.stack([lo, hi], axis=1).reshape(count, 8, lanes).astype(bf16)
        )
        returned[part] = over_ep(ret_send, ret, b_s, b_r, part, -1)

    give_back(FAR)
    give_back(NEAR)
    ret[0] = ret_send[0]
    high = combine.astype(bf16)
    left_over = combine - high.astype(f32)
    mid = left_over.astype(bf16)
    low = (left_over - mid.astype(f32)).astype(bf16)
    for part in (NEAR, FAR):
        returned[part].wait_recv()
    back = ret[...].reshape(cols, lanes)
    mix = mm(high, back) + mm(mid, back) + mm(low, back)
    out_ref[:, :lanes] = (stream[:, :lanes] + mix[:seqs]).astype(bf16)
    out_ref[:, lanes:] = (stream[:, lanes:] + mix[seqs:]).astype(bf16)

    for copy in copies:
        copy.wait_send()
    for some in (dispatched, g_copies, p_copies, t_copies, returned):
        for copy in some.values():
            copy.wait_send()


def body(n_ep, n_tp, *args):
    (
        tokens, norm_gain, post_gain, w_query, w_key, w_value, w_forget, w_output,
        key_cache, value_cache, gate_cache, lengths, routes, route_logits, w_gate, w_up, w_down,
    ) = args
    seqs, width = tokens.shape
    hd, span = key_cache.shape[2:]
    heads = gate_cache.shape[1]
    own = width // n_tp
    operands = (
        tokens, norm_gain.reshape(1, width), post_gain.reshape(1, width),
        w_query, w_key.T, w_value.T, w_forget.T, w_output,
        key_cache.reshape(seqs * hd, span), value_cache.reshape(seqs * hd, span), gate_cache,
        lengths.reshape(1, seqs), routes.T, route_logits.T, w_gate[0].T, w_up[0].T, w_down[0],
    )
    slots = 4 * n_ep
    dma = pltpu.SemaphoreType.DMA
    kvf_rows = operands[4].shape[0] + operands[5].shape[0] + operands[6].shape[0]
    kvf = jax.ShapeDtypeStruct((kvf_rows, width), bf16)
    held = operands[:4] + (kvf,) + operands[7:]
    scratch = [pltpu.VMEM(a.shape, a.dtype) for a in held] + [
        pltpu.VMEM((seqs * heads, span), bf16),
        pltpu.VMEM((n_tp, seqs, own), bf16),
        pltpu.VMEM((n_tp, seqs, own), bf16),
        pltpu.VMEM((n_ep, 8, own // 2), bf16),
        pltpu.VMEM((n_ep, 8, own // 2), bf16),
        pltpu.VMEM((n_tp, slots, own), bf16),
        pltpu.VMEM((n_tp // 2, slots, own), bf16),
        pltpu.VMEM((n_tp // 2, slots, own), bf16),
        pltpu.VMEM((n_tp // 2, slots, own), bf16),
        pltpu.VMEM((n_tp // 2, slots, own), bf16),
        pltpu.VMEM((n_ep, 8, own // 2), bf16),
        pltpu.VMEM((n_ep, 8, own // 2), bf16),
        dma((32,)),
        dma((n_tp,)), dma((n_tp,)),
        dma((2,)), dma((2,)),
        dma((2, n_tp)), dma((2, n_tp)),
        dma((n_tp // 2,)), dma((n_tp // 2,)),
        dma((2, n_tp // 2)), dma((2, n_tp // 2)),
        dma((2,)), dma((2,)),
    ]
    return pl.pallas_call(
        functools.partial(kernel, n_ep, n_tp),
        out_shape=pltpu.VMEM((seqs, own), bf16),
        in_specs=[pl.BlockSpec(memory_space=pltpu.HBM)] * len(operands),
        out_specs=pl.BlockSpec(memory_space=pltpu.VMEM),
        scratch_shapes=scratch,
        compiler_params=pltpu.CompilerParams(
            collective_id=0, has_side_effects=True, vmem_limit_bytes=54 * 1024 * 1024
        ),
        name="layer",
    )(*operands)


def solution(mesh):
    in_specs = (
        P("ep", None),
        P(),
        P(),
        P(None, "tp"),
        P(None, "tp"),
        P(None, "tp"),
        P(),
        P("tp", None),
        P("ep", "tp", None, None),
        P("ep", "tp", None, None),
        P("ep", "tp", None),
        P("ep"),
        P("ep", None),
        P("ep", None),
        P("ep", None, "tp"),
        P("ep", None, "tp"),
        P("ep", "tp", None),
    )
    step = functools.partial(body, mesh.shape["ep"], mesh.shape["tp"])
    return jax.shard_map(
        step, mesh=mesh, in_specs=in_specs, out_specs=P("ep", "tp"), check_vma=False
    )
```
